32 devices in a mesh: ep: 8 (over z, core), tp: 4 (over y, x).
Axes of the slice: x: 2, y: 2, z: 4, core: 2. Of those that a mesh axis runs over, the one named last changes fastest.
Arguments:
- q_latent: bfloat16 [4096, 512], P('ep'), may hold values from -6 to 6
- kv_latent: bfloat16 [4096, 256], P('ep'), may hold values from -6 to 6
- rope_key: bfloat16 [4096, 32], P('ep'), may hold values from -400 to 400
- q_gain: bfloat16 [512], replicated, may hold values from 0.099609375 to 1.8984375
- kv_gain: bfloat16 [256], replicated, may hold values from 0.099609375 to 1.8984375
- w_q_nope: bfloat16 [512, 1024], P(None, 'tp'), may hold values from -0.25 to 0.25
- w_q_rope: bfloat16 [512, 512], P(None, 'tp'), may hold values from -0.25 to 0.25
- w_k_nope: bfloat16 [256, 1024], P(None, 'tp'), may hold values from -0.375 to 0.375
- w_value: bfloat16 [256, 1024], P(None, 'tp'), may hold values from -0.375 to 0.375
- w_out: bfloat16 [1024, 2048], P('tp'), may hold values from -5.375 to 5.375
- tokens_b: bfloat16 [1024, 2048], P('ep'), may hold values from -6 to 6
- norm_gain_b: bfloat16 [2048], replicated, may hold values from 0.099609375 to 1.8984375
- routes: int32 [1024, 2], P('ep'), may hold values from 0 to 7, all different within a row; in each aligned block of 128 rows (0 to 127, 128 to 255, ...) at most 48 rows name the same one
- route_logits: float32 [1024, 2], P('ep'), may hold values from -6 to 6
- w_gate: bfloat16 [8, 2048, 4096], P('ep', None, 'tp'), may hold values from -0.125 to 0.125
- w_up: bfloat16 [8, 2048, 4096], P('ep', None, 'tp'), may hold values from -0.125 to 0.125
- w_down: bfloat16 [8, 4096, 2048], P('ep', 'tp'), may hold values from -0.125 to 0.125
Outputs:
- mixer_out: bfloat16 [4096, 2048], P(('ep', 'tp'))
- expert_mix: bfloat16 [1024, 2048], P('ep', 'tp')
The draws below stay inside these ranges and needn't reach their ends.
Inputs may be any that keep to these rules, and one draw needn't show every extreme that they name: `routes`: each row names two different experts. In each aligned block of 128 rows (the rows of one index of ep) no expert is named by more than 48 rows, and in every draw some expert is named by exactly 48 rows of some block.
All inputs are finite; a program needn't handle non-finite values.
Results may differ from the reference program's by a relative error of at most 0.022.
The reference program's roundings to bfloat16 on the way count: a program that leaves them out, or rounds other values in their place, can miss the bound.
Values may be sent and summed in bfloat16 or wider, within the bound.
A program may use at most 128 MiB of HBM per device.

```python
import math
import jax
import jax.numpy as jnp
import numpy as np
from jax import lax

D = 2048
HEADS = 16
NOPE = 64
ROPE = 32
VDIM = 64
QLAT = 512
KVLAT = 256
FFE = 4096
R_B = 128
TOK_A = 4096
TOK_B = 1024
EXPERTS = 8
CAP = 48
N_EP = 8
N_TP = 4


def draw_rope_key(key, part):
    base = jax.random.normal(jax.random.fold_in(key, 11), (TOK_A, ROPE), jnp.float32)
    return jnp.clip(base, -400.0, 400.0).astype(jnp.bfloat16)


def with_spikes(drawn, stream_key, source, target, blocks, factor):
    owner, partner = [(jnp.arange(drawn.shape[axis_at]) // (drawn.shape[axis_at] // blocks)).reshape([-1 if axis == axis_at else 1 for axis in range(drawn.ndim)]) for axis_at in (source, target)]
    chosen = jax.random.permutation(stream_key, blocks)[partner]
    strong = (owner == chosen) | (owner == (partner + blocks // 2) % blocks)
    return jnp.where(strong, factor * drawn, drawn)


def level_of(own_key, extent, cuts, low, top_value):
    level = 1.0
    for axis_at, blocks in cuts:
        steps = jax.random.uniform(jax.random.fold_in(jax.random.fold_in(own_key, 6), axis_at), (blocks,), jnp.float32, low / len(cuts), top_value / len(cuts))
        level = level * jnp.repeat(jnp.exp(steps), extent[axis_at] // blocks).reshape((-1,) + (1,) * (len(extent) - 1 - axis_at))
    return level


def assign_block(stream_key, own, number, rows, number_of, top, most, slope):
    ranking = jax.random.permutation(stream_key, number_of)
    crowded, usual = load_shares(number_of, rows * top, most, slope, True), load_shares(number_of, rows * top, most, slope, False)
    places = jnp.arange(number_of)

    def named(sizes, turn):
        used = int((sizes > 0).sum())
        fixed = max(1, used // 4)
        passed = fixed + (places - fixed + turn * (used - fixed)) % max(1, number_of - fixed)
        return jnp.zeros((number_of,), jnp.int32).at[ranking[jnp.where(places < fixed, places, passed)]].set(jnp.asarray(sizes, jnp.int32))

    sizes = jnp.where(number % 4 == 0, named(crowded, number // 4), named(usual, number - number // 4 - 1))
    mixed = jax.random.permutation(jax.random.fold_in(own, 3), number_of)
    donor, sink = mixed[0:number_of // 2 * 2:2], mixed[1:number_of // 2 * 2:2]
    margin = jnp.minimum(sizes[donor] - 1, most - sizes[sink]) // 2
    margin = jnp.where((donor == ranking[0]) | (sink == ranking[0]) | (sizes[sink] == 0), 0, jnp.maximum(margin, 0))
    passed = jax.random.randint(jax.random.fold_in(own, 4), (number_of // 2,), 0, 1 << 20) % (margin + 1)
    sizes = sizes.at[donor].add(-passed).at[sink].add(passed)
    items = jnp.searchsorted(jnp.cumsum(sizes), jnp.arange(rows * top), side="right").astype(jnp.int32)
    grid = items.reshape(top, rows).T
    grid = grid[jax.random.permutation(jax.random.fold_in(own, 1), rows)]
    turn = jax.random.randint(jax.random.fold_in(own, 2), (rows, 1), 0, top)
    return jnp.take_along_axis(grid, (jnp.arange(top)[None, :] + turn) % top, axis=1)


def load_shares(count, total, reach, skew, full):
    loads = [(1 << 20) // math.isqrt(grade ** skew) + 1 for grade in range(1, count + 1)]
    largest = reach if full else min(reach, max(-(-total // count), total * loads[0] // sum(loads)))
    least = 1 if total - largest >= count - 1 else 0
    given, rest = [largest] + [least] * (count - 1), total - largest - least * (count - 1)
    while rest > 0:
        candidates = [i for i in range(1, count) if given[i] < largest] or [i for i in range(1, count) if given[i] < reach]
        pool, remaining = sum([loads[i] for i in candidates]), rest
        for i in candidates:
            more = min(reach - given[i], max(1, remaining * loads[i] // pool), rest)
            given[i] = given[i] + more
            rest = rest - more
    return np.array(given)


def centred(key, shape, scale, most, cuts=(), kind=jnp.bfloat16):
    entries = jax.random.normal(key, shape, jnp.float32) * scale
    if len(cuts) > 0:
        entries = level_of(key, shape, cuts, -0.22, 0.18) * entries
    return jnp.clip(entries, min=-most, max=most).astype(kind)


def noise_with(key, extent, width, bound, pieces, heavy, kind=jnp.bfloat16):
    drawn = width * jax.random.normal(key, extent, jnp.float32)
    if pieces:
        drawn = drawn * level_of(key, extent, pieces, -0.22, 0.18)
    return jnp.clip(with_spikes(drawn, jax.random.fold_in(key, 3), *heavy), -bound, bound).astype(kind)


def setup_inputs(seed: int = 0) -> dict:
    keys = jax.random.split(jax.random.key(seed), 18)
    q_latent = centred(keys[0], (TOK_A, QLAT), 1.0, 6.0, ((0, 8),))
    kv_latent = centred(keys[1], (TOK_A, KVLAT), 1.0, 6.0, ((0, 8),))
    rope_key = draw_rope_key(jax.random.fold_in(keys[17], 71), 0)
    q_gain = jnp.clip(1.0 + 0.18 * jax.random.normal(keys[3], (QLAT,), jnp.float32), 0.099609375, 1.8984375).astype(jnp.bfloat16)
    kv_gain = jnp.clip(1.0 + 0.18 * jax.random.normal(keys[4], (KVLAT,), jnp.float32), 0.099609375, 1.8984375).astype(jnp.bfloat16)
    w_q_nope = centred(keys[5], (QLAT, HEADS * NOPE), QLAT ** -0.5, 0.25, ((1, 4),))
    w_q_rope = centred(keys[6], (QLAT, HEADS * ROPE), QLAT ** -0.5, 0.25, ((1, 4),))
    w_k_nope = centred(keys[7], (KVLAT, HEADS * NOPE), KVLAT ** -0.5, 0.375, ((1, 4),))
    w_value = centred(keys[8], (KVLAT, HEADS * VDIM), KVLAT ** -0.5, 0.375, ((1, 4),))
    w_out = centred(keys[9], (HEADS * VDIM, D), 0.9, 5.375, ((0, 4),))
    tokens_b = centred(keys[10], (TOK_B, D), 1.0, 6.0, ((0, 8),))
    norm_gain_b = jnp.clip(1.0 + 0.18 * jax.random.normal(keys[11], (D,), jnp.float32), 0.099609375, 1.8984375).astype(jnp.bfloat16)
    routes_keys = jax.random.split(jax.random.fold_in(keys[12], 1), TOK_B // R_B)
    routes_turns = jax.random.permutation(jax.random.fold_in(keys[12], 3), TOK_B // R_B)
    routes = jax.vmap(lambda own, number: assign_block(jax.random.fold_in(keys[12], 2), own, number, R_B, EXPERTS, 2, CAP, 2))(routes_keys, routes_turns).reshape((TOK_B, 2))
    route_logits = centred(keys[13], (TOK_B, 2), 1.5, 6.0, ((0, 8),), jnp.float32)
    w_gate = centred(keys[14], (EXPERTS, D, FFE), D ** -0.5, 0.125, ((0, 8), (2, 4)))
    w_up = centred(keys[15], (EXPERTS, D, FFE), D ** -0.5, 0.125, ((0, 8), (2, 4)))
    w_down = noise_with(keys[16], (EXPERTS, FFE, D), FFE ** -0.5, 0.125, ((0, 8), (1, 4)), (1, 2, 4, 2.0))
    return dict(q_latent=q_latent, kv_latent=kv_latent, rope_key=rope_key, q_gain=q_gain, kv_gain=kv_gain, w_q_nope=w_q_nope, w_q_rope=w_q_rope, w_k_nope=w_k_nope, w_value=w_value, w_out=w_out, tokens_b=tokens_b, norm_gain_b=norm_gain_b, routes=routes, route_logits=route_logits, w_gate=w_gate, w_up=w_up, w_down=w_down)


EPSILON = 1e-06

def rms_rows(values, gain):
    wide = values.astype(jnp.float32)
    scaled = wide * lax.rsqrt(lax.optimization_barrier(jnp.mean(wide * wide, axis=-1, keepdims=True)) + EPSILON)
    return (scaled * gain.astype(jnp.float32)).astype(jnp.bfloat16)

def rotate(values, places):
    half = values.shape[-1] // 2
    freqs = 10000.0 ** (-jnp.arange(half, dtype=jnp.float32) / half)
    angles = places.astype(jnp.float32)[:, None] * freqs[None, :]
    cosine = jnp.cos(angles)[:, None, :]
    sine = jnp.sin(angles)[:, None, :]
    first = values[..., :half]
    second = values[..., half:]
    return jnp.concatenate([first * cosine - second * sine, first * sine + second * cosine], axis=-1)

def add_group(acc, operands):
    part = jnp.dot(operands[0], operands[1], preferred_element_type=jnp.float32).astype(jnp.bfloat16)
    part = lax.optimization_barrier(part)
    return (acc + part.astype(jnp.float32), None)

def reference(q_latent, kv_latent, rope_key, q_gain, kv_gain, w_q_nope, w_q_rope, w_k_nope, w_value, w_out, tokens_b, norm_gain_b, routes, route_logits, w_gate, w_up, w_down):
    total = q_latent.shape[0]
    places = jnp.arange(total, dtype=jnp.int32)
    q_normed = rms_rows(q_latent, q_gain)
    q_nope = jnp.dot(q_normed, w_q_nope, preferred_element_type=jnp.float32).astype(jnp.bfloat16)
    q_nope = q_nope.reshape(total, HEADS, NOPE)
    q_turn = jnp.dot(q_normed, w_q_rope, preferred_element_type=jnp.float32).reshape(total, HEADS, ROPE)
    q_rope = rotate(q_turn, places).astype(jnp.bfloat16)
    kv_normed = rms_rows(kv_latent, kv_gain)
    k_nope = jnp.dot(kv_normed, w_k_nope, preferred_element_type=jnp.float32).astype(jnp.bfloat16)
    k_nope = k_nope.reshape(total, HEADS, NOPE)
    values = jnp.dot(kv_normed, w_value, preferred_element_type=jnp.float32).astype(jnp.bfloat16)
    values = values.reshape(total, HEADS, VDIM)
    k_rope = rotate(rope_key.astype(jnp.float32)[:, None, :], places)[:, 0].astype(jnp.bfloat16)
    scale = (NOPE + ROPE) ** (-0.5)

    def one_head(operands):
        head_q, head_r, head_k, head_v = operands
        scores = jnp.dot(head_q, head_k.T, preferred_element_type=jnp.float32)
        scores = (scores + jnp.dot(head_r, k_rope.T, preferred_element_type=jnp.float32)) * scale
        top = lax.optimization_barrier(jnp.max(scores, axis=-1, keepdims=True))
        weights = jnp.exp(scores - top)
        total_w = lax.optimization_barrier(jnp.sum(weights, axis=-1, keepdims=True))
        mixed = jnp.dot(weights.astype(jnp.bfloat16), head_v, preferred_element_type=jnp.float32) / total_w
        return mixed.astype(jnp.bfloat16)
    heads_out = lax.map(one_head, (q_nope.transpose(1, 0, 2), q_rope.transpose(1, 0, 2), k_nope.transpose(1, 0, 2), values.transpose(1, 0, 2)))
    group = HEADS // N_TP
    grouped = heads_out.reshape(N_TP, group, total, VDIM).transpose(0, 2, 1, 3).reshape(N_TP, total, group * VDIM)
    out_rows = w_out.reshape(N_TP, group * VDIM, D)
    summed, _ = lax.scan(add_group, jnp.zeros((total, D), jnp.float32), (grouped, out_rows))
    mixer_out = summed.astype(jnp.bfloat16)
    rows_b = tokens_b.shape[0]
    normed_b = rms_rows(tokens_b, norm_gain_b)
    weights_b = jax.nn.softmax(route_logits.astype(jnp.float32), axis=-1)
    flat = routes.reshape(-1).astype(jnp.int32)
    assigned = flat.shape[0]
    onehot = (flat[:, None] == jnp.arange(EXPERTS, dtype=jnp.int32)[None, :]).astype(jnp.int32)
    slot = lax.optimization_barrier(jnp.sum((jnp.cumsum(onehot, axis=0) - 1) * onehot, axis=1)).astype(jnp.int32)
    room = N_EP * CAP
    table = jnp.full((EXPERTS, room), assigned, jnp.int32).at[flat, slot].set(jnp.arange(assigned, dtype=jnp.int32))
    padded = jnp.concatenate([normed_b, jnp.zeros((1, D), jnp.bfloat16)], axis=0)
    slices = FFE // N_TP

    def one_expert(operands):
        picks, gate_w, up_w, down_w = operands
        rows = padded[picks // 2]
        gate = jnp.dot(rows, gate_w, preferred_element_type=jnp.float32)
        up = jnp.dot(rows, up_w, preferred_element_type=jnp.float32)
        hidden = (jax.nn.silu(gate) * up).astype(jnp.bfloat16)
        hidden = hidden.reshape(room, N_TP, slices).transpose(1, 0, 2)
        down = down_w.reshape(N_TP, slices, D)
        total_e, _ = lax.scan(add_group, jnp.zeros((room, D), jnp.float32), (hidden, down))
        return total_e.astype(jnp.bfloat16)
    expert_out = lax.map(one_expert, (table, w_gate, w_up, w_down)).reshape(EXPERTS * room, D)
    where = (flat * room + slot).reshape(rows_b, 2)
    picked = expert_out[where].astype(jnp.float32)
    expert_mix = lax.optimization_barrier(jnp.sum(picked * weights_b[:, :, None], axis=1)).astype(jnp.bfloat16)
    return (mixer_out, expert_mix)
```

```python
import functools
import math

import jax
import jax.numpy as jnp
from jax import lax
from jax.experimental import pallas as pl
from jax.experimental.pallas import tpu as pltpu
from jax.sharding import PartitionSpec as P

NOPE = 64
ROPE = 32
VDIM = 64
LANES = 128
EPSILON = 1e-06
BF = jnp.bfloat16
F32 = jnp.float32


def rms_rows(values, gain):
    wide = values.astype(F32)
    scaled = wide * lax.rsqrt(jnp.mean(wide * wide, axis=-1, keepdims=True) + EPSILON)
    return (scaled * gain.astype(F32)).astype(BF)


def angle_tables(places):
    half = ROPE // 2
    freqs = 10000.0 ** (-jnp.arange(half, dtype=F32) / half)
    angles = places.astype(F32)[:, None] * freqs[None, :]
    return jnp.cos(angles), jnp.sin(angles)


def attention_kernel(heads, q_ref, kv_ref, w_ref, out_ref, k_buf, v_buf):
    keys = kv_ref.shape[0]
    rows = q_ref.shape[1]
    scale = (NOPE + ROPE) ** (-0.5) * math.log2(math.e)
    chunk = 512
    q_block = min(256, rows)
    k_block = 1024
    wide = heads * LANES

    def project(c, _):
        here = pl.ds(pl.multiple_of(c * chunk, chunk), chunk)
        up = jnp.dot(kv_ref[here, :], w_ref[...], preferred_element_type=F32)
        lane = lax.broadcasted_iota(jnp.int32, (chunk, LANES), 1)
        for h in range(heads):
            k_buf[h, here, :] = up[:, h * LANES : (h + 1) * LANES].astype(BF)
            v = up[:, wide + h * LANES : wide + (h + 1) * LANES]
            v_buf[h, here, :] = jnp.where(lane < VDIM, v, 1.0).astype(BF)
        return 0

    lax.fori_loop(0, keys // chunk, project, 0)

    def attend(step, _):
        h = step // (rows // q_block)
        b = step % (rows // q_block)
        here = pl.ds(pl.multiple_of(b * q_block, q_block), q_block)
        q = q_ref[h, here, :]
        top = jnp.full((q_block, 1), -jnp.inf, F32)
        acc = jnp.zeros((q_block, LANES), F32)
        for j in range(keys // k_block):
            at = slice(j * k_block, (j + 1) * k_block)
            s = lax.dot_general(
                q, k_buf[h, at, :], (((1,), (1,)), ((), ())), preferred_element_type=F32
            )
            new_top = jnp.maximum(top, jnp.max(s, axis=-1, keepdims=True))
            p = jnp.exp2((s - new_top) * scale).astype(BF)
            pv = jnp.dot(p, v_buf[h, at, :], preferred_element_type=F32)
            if j == 0:
                acc = pv
            else:
                acc = acc * jnp.exp2((top - new_top) * scale) + pv
            top = new_top
        out_ref[h, here, :] = (acc[:, :VDIM] / acc[:, VDIM : VDIM + 1]).astype(BF)
        return 0

    lax.fori_loop(0, heads * (rows // q_block), attend, 0)


def attention(q, kv, w):
    heads, rows, _ = q.shape
    keys = kv.shape[0]
    flops = 4 * heads * rows * keys * 256
    return pl.pallas_call(
        functools.partial(attention_kernel, heads),
        out_shape=jax.ShapeDtypeStruct((heads, rows, VDIM), BF),
        in_specs=[pl.BlockSpec(memory_space=pltpu.VMEM)] * 3,
        out_specs=pl.BlockSpec(memory_space=pltpu.VMEM),
        scratch_shapes=[
            pltpu.VMEM((heads, keys, LANES), BF),
            pltpu.VMEM((heads, keys, LANES), BF),
        ],
        compiler_params=pltpu.CompilerParams(vmem_limit_bytes=48 * 1024 * 1024),
        cost_estimate=pl.CostEstimate(
            flops=flops, bytes_accessed=8 * 1024 * 1024, transcendentals=heads * rows * keys
        ),
        name="attention",
    )(q, kv, w)


def lay_heads(weights, heads, width, offset):
    depth = weights.shape[0]
    split = weights.reshape(depth, heads, width)
    return jnp.pad(split, ((0, 0), (0, 0), (offset, LANES - width - offset)))


def shards(
    q_latent,
    kv_latent,
    rope_key,
    q_gain,
    kv_gain,
    w_q_nope,
    w_q_rope,
    w_k_nope,
    w_value,
    w_out,
    tokens_b,
    norm_gain_b,
    routes,
    route_logits,
    w_gate,
    w_up,
    w_down,
):
    n_ep = lax.axis_size("ep")
    n_tp = lax.axis_size("tp")
    e_at = lax.axis_index("ep")
    t_at = lax.axis_index("tp")
    own_rows = q_latent.shape[0]
    heads = w_q_nope.shape[1] // NOPE
    rows_b = tokens_b.shape[0]
    width = tokens_b.shape[1]
    half = ROPE // 2

    part = own_rows // n_tp
    kv_part = lax.dynamic_slice_in_dim(kv_latent, t_at * part, part, 0)
    rope_part = lax.dynamic_slice_in_dim(rope_key, t_at * part, part, 0).astype(F32)
    places = e_at * own_rows + t_at * part + jnp.arange(part, dtype=jnp.int32)
    cosine, sine = angle_tables(places)
    first, second = rope_part[:, :half], rope_part[:, half:]
    sent = jnp.concatenate(
        [
            rms_rows(kv_part, kv_gain),
            (first * cosine - second * sine).astype(BF),
            (first * sine + second * cosine).astype(BF),
        ],
        axis=1,
    )
    kv_all = lax.all_gather(sent, ("ep", "tp"), axis=0, tiled=True)

    part_b = rows_b // n_tp
    tok_part = lax.dynamic_slice_in_dim(tokens_b, t_at * part_b, part_b, 0)
    route_part = lax.dynamic_slice_in_dim(routes, t_at * part_b, part_b, 0)
    logit_part = lax.dynamic_slice_in_dim(route_logits, t_at * part_b, part_b, 0)
    weights_b = jax.nn.softmax(logit_part, axis=-1)
    high = weights_b.astype(BF)
    low = (weights_b - high.astype(F32)).astype(BF)
    extra = jnp.concatenate(
        [route_part.astype(BF), high, low, jnp.zeros((part_b, LANES - 6), BF)], axis=1
    )
    sent_b = jnp.concatenate([rms_rows(tok_part, norm_gain_b), extra], axis=1)
    tok_all = lax.all_gather(sent_b, ("ep", "tp"), axis=0, tiled=True)

    q_normed = rms_rows(q_latent, q_gain)
    w_nope = lay_heads(w_q_nope, heads, NOPE, 0)
    w_rope = lay_heads(w_q_rope, heads, ROPE, NOPE)
    turn = w_q_rope.reshape(-1, heads, ROPE)
    turned = jnp.concatenate([-turn[..., half:], turn[..., :half]], axis=-1)
    w_turned = jnp.pad(turned, ((0, 0), (0, 0), (NOPE, LANES - NOPE - ROPE)))
    cos_q, sin_q = angle_tables(e_at * own_rows + jnp.arange(own_rows, dtype=jnp.int32))
    ones = jnp.ones((own_rows, NOPE), F32)
    tail = jnp.zeros((own_rows, LANES - NOPE - ROPE), F32)
    cos_row = jnp.concatenate([ones, cos_q, cos_q, tail], axis=1)
    sin_row = jnp.concatenate([0.0 * ones, sin_q, sin_q, tail], axis=1)
    plain = jnp.einsum("rd,dhl->hrl", q_normed, w_nope + w_rope, preferred_element_type=F32)
    swapped = jnp.einsum("rd,dhl->hrl", q_normed, w_turned, preferred_element_type=F32)
    q = (plain * cos_row + swapped * sin_row).astype(BF)

    place = jnp.pad(jnp.eye(ROPE, dtype=BF), ((0, 0), (NOPE, LANES - NOPE - ROPE)))
    place = jnp.broadcast_to(place[:, None, :], (ROPE, heads, LANES))
    w_keys = jnp.concatenate([lay_heads(w_k_nope, heads, NOPE, 0), place], axis=0)
    w_vals = jnp.pad(lay_heads(w_value, heads, VDIM, 0), ((0, ROPE), (0, 0), (0, 0)))
    w_kv = jnp.concatenate(
        [w_keys.reshape(-1, heads * LANES), w_vals.reshape(-1, heads * LANES)], axis=1
    )
    attended = attention(q, kv_all, w_kv)
    attended = attended.transpose(1, 0, 2).reshape(own_rows, heads * VDIM)
    mixer_out = lax.psum_scatter(
        jnp.dot(attended, w_out, preferred_element_type=F32).astype(BF),
        "tp",
        scatter_dimension=0,
        tiled=True,
    )

    room = 3 * rows_b // n_ep
    total_b = tok_all.shape[0]
    info = tok_all[:, width : width + LANES].astype(F32)
    me = e_at.astype(F32)
    hit_0 = (info[:, 0] == me).astype(F32)
    hit_1 = (info[:, 1] == me).astype(F32)
    hit = hit_0 + hit_1
    weight = hit_0 * (info[:, 2] + info[:, 4]) + hit_1 * (info[:, 3] + info[:, 5])
    order = jnp.arange(rows_b)
    before = (order[:, None] < order[None, :]).astype(BF)
    slot = jnp.dot(hit.reshape(n_ep, rows_b).astype(BF), before, preferred_element_type=F32)
    row = slot + (jnp.arange(n_ep, dtype=F32) * room)[:, None]
    row = jnp.where(hit > 0, row.reshape(total_b), -1.0)
    index = jnp.arange(n_ep * room, dtype=F32)
    chosen = index[:, None] == row[None, :]
    pick = chosen.astype(BF)
    row_weight = jnp.sum(jnp.where(chosen, weight[None, :], 0.0), axis=1, keepdims=True)
    piece = jnp.dot(pick, tok_all[:, :width], preferred_element_type=F32).astype(BF)
    gate = jnp.dot(piece, w_gate[0], preferred_element_type=F32)
    up = jnp.dot(piece, w_up[0], preferred_element_type=F32)
    hidden = (jax.nn.silu(gate) * up).astype(BF)
    term = jnp.dot(hidden, w_down[0], preferred_element_type=F32)
    scaled = (term * row_weight).astype(BF)
    share = width // n_tp
    spread = jnp.einsum(
        "reb,rjc->ejbc",
        pick.reshape(n_ep * room, n_ep, rows_b),
        scaled.reshape(n_ep * room, n_tp, share),
        preferred_element_type=F32,
    ).astype(BF)
    expert_mix = lax.psum_scatter(
        spread.reshape(n_ep * n_tp * rows_b, share), ("ep", "tp"), scatter_dimension=0, tiled=True
    )
    return (mixer_out, expert_mix)


def solution(mesh):
    placed = (
        P("ep", None),
        P("ep", None),
        P("ep", None),
        P(),
        P(),
        P(None, "tp"),
        P(None, "tp"),
        P(None, "tp"),
        P(None, "tp"),
        P("tp", None),
        P("ep", None),
        P(),
        P("ep", None),
        P("ep", None),
        P("ep", None, "tp"),
        P("ep", None, "tp"),
        P("ep", "tp", None),
    )
    return jax.shard_map(
        shards,
        mesh=mesh,
        in_specs=placed,
        out_specs=(P(("ep", "tp"), None), P("ep", "tp")),
        check_vma=False,
    )
```

```python
import functools
import math

import jax
import jax.numpy as jnp
from jax import lax
from jax.experimental import pallas as pl
from jax.experimental.pallas import tpu as pltpu
from jax.sharding import PartitionSpec as P

NOPE = 64
ROPE = 32
VDIM = 64
LANES = 128
EPSILON = 1e-06
BF = jnp.bfloat16
F32 = jnp.float32


def rms_rows(values, gain):
    wide = values.astype(F32)
    scaled = wide * lax.rsqrt(jnp.mean(wide * wide, axis=-1, keepdims=True) + EPSILON)
    return (scaled * gain.astype(F32)).astype(BF)


def angle_tables(places):
    half = ROPE // 2
    freqs = 10000.0 ** (-jnp.arange(half, dtype=F32) / half)
    angles = places.astype(F32)[:, None] * freqs[None, :]
    return jnp.cos(angles), jnp.sin(angles)


MESH = pl.DeviceIdType.MESH


def remote(src, dst, send, recv, ep, tp):
    return pltpu.make_async_remote_copy(
        src_ref=src,
        dst_ref=dst,
        send_sem=send,
        recv_sem=recv,
        device_id={"ep": ep, "tp": tp},
        device_id_type=MESH,
    )


def loop(count, body, start=0):
    def step(i, c):
        body(i)
        return c

    lax.fori_loop(start, count, step, 0)


class Gather:
    def __init__(self, n_ep, n_tp, own, buf, local, recv, send_z, send_t, send_c):
        self.n_tp, self.nz = n_tp, n_ep // 2
        self.own, self.buf, self.local = own, buf, local
        self.recv, self.send_z, self.send_t, self.send_c = recv, send_z, send_t, send_c
        ep = lax.axis_index("ep")
        self.z, self.core, self.t = ep // 2, ep % 2, lax.axis_index("tp")
        self.ep = ep

    def slot(self, z, core, t):
        return (z * 2 + core) * self.n_tp + t

    def at_z(self, d):
        return (self.z + self.nz - d) % self.nz

    def at_t(self, d):
        return (self.t + self.n_tp - d) % self.n_tp

    def copy_z(self, d):
        me = self.slot(self.z, self.core, self.t)
        to = (self.z + d) % self.nz
        return remote(
            self.own, self.buf.at[me], self.send_z.at[d], self.recv.at[me], to * 2 + self.core, self.t
        )

    def copy_t(self, dz, d):
        s = self.slot(self.at_z(dz), self.core, self.t)
        to = (self.t + d) % self.n_tp
        return remote(
            self.buf.at[s], self.buf.at[s], self.send_t.at[dz * self.n_tp + d], self.recv.at[s], self.ep, to
        )

    def copy_c(self, dz, d):
        s = self.slot(self.at_z(dz), self.core, self.at_t(d))
        return remote(
            self.buf.at[s],
            self.buf.at[s],
            self.send_c.at[dz * self.n_tp + d],
            self.recv.at[s],
            self.z * 2 + 1 - self.core,
            self.t,
        )

    def landed(self, s):
        remote(self.own, self.buf.at[s], self.local, self.recv.at[s], self.ep, self.t).wait_recv()

    def start(self):
        loop(self.nz, lambda d: self.copy_z(d).start(), 1)
        me = self.slot(self.z, self.core, self.t)
        mine = pltpu.make_async_copy(self.own, self.buf.at[me], self.local)
        mine.start()
        mine.wait()

    def over_tp(self):
        def one(dz):
            @pl.when(dz > 0)
            def _():
                self.landed(self.slot(self.at_z(dz), self.core, self.t))

            loop(self.n_tp, lambda d: self.copy_t(dz, d).start(), 1)
            self.copy_c(dz, 0).start()

        loop(self.nz, one)

    def to_sibling(self):
        def one(dz):
            def inner(d):
                self.landed(self.slot(self.at_z(dz), self.core, self.at_t(d)))
                self.copy_c(dz, d).start()

            loop(self.n_tp, inner, 1)

        loop(self.nz, one)

    def finish(self):
        def one(dz):
            def inner(d):
                self.landed(self.slot(self.at_z(dz), 1 - self.core, self.at_t(d)))
                self.copy_c(dz, d).wait_send()

            loop(self.n_tp, inner)
            loop(self.n_tp, lambda d: self.copy_t(dz, d).wait_send(), 1)

        loop(self.nz, one)
        loop(self.nz, lambda d: self.copy_z(d).wait_send(), 1)


def greet(n_ep, n_tp, every_ep):
    ep, t = lax.axis_index("ep"), lax.axis_index("tp")
    barrier = pltpu.get_barrier_semaphore()

    def hello(e, tp):
        pl.semaphore_signal(barrier, inc=1, device_id={"ep": e, "tp": tp}, device_id_type=MESH)

    loop(n_tp, lambda d: hello(ep, (t + d) % n_tp), 1)
    if every_ep:
        loop(n_ep, lambda d: hello((ep + d) % n_ep, t), 1)
        pl.semaphore_wait(barrier, n_tp + n_ep - 2)
    else:
        nz = n_ep // 2
        loop(nz, lambda d: hello((ep // 2 + d) % nz * 2 + ep % 2, t), 1)
        hello(ep // 2 * 2 + 1 - ep % 2, t)
        pl.semaphore_wait(barrier, n_tp + nz - 1)


def attention_kernel(
    heads, n_ep, n_tp, sent_ref, tok_ref, q_ref, w_ref, out_ref, tok_out, kv_buf, k_buf, v_buf, *sems
):
    part, lat = sent_ref.shape[0], w_ref.shape[0]
    keys = n_ep * n_tp * part
    rows = q_ref.shape[1]
    scale = (NOPE + ROPE) ** (-0.5) * math.log2(math.e)
    q_block = min(256, rows)
    k_block = 1024
    wide = heads * LANES
    latents = Gather(n_ep, n_tp, sent_ref, kv_buf, *sems[:5])
    tokens = Gather(n_ep, n_tp, tok_ref, tok_out, *sems[5:])
    greet(n_ep, n_tp, False)
    latents.start()
    latents.over_tp()
    tokens.start()
    latents.to_sibling()
    latents.finish()
    tokens.over_tp()
    group = max(1, 512 // part)
    chunk = group * part

    def project(c):
        here = pl.ds(pl.multiple_of(c * chunk, chunk), chunk)
        block = kv_buf[pl.ds(c * group, group)].reshape(chunk, kv_buf.shape[2])
        up = jnp.dot(block[:, :lat], w_ref[...], preferred_element_type=F32)
        turned = block[:, lat:].astype(F32)
        lane = lax.broadcasted_iota(jnp.int32, (chunk, LANES), 1)
        for h in range(heads):
            k_buf[h, here, :] = (up[:, h * LANES : (h + 1) * LANES] + turned).astype(BF)
            v = up[:, wide + h * LANES : wide + (h + 1) * LANES]
            v_buf[h, here, :] = jnp.where(lane < VDIM, v, 1.0).astype(BF)

    loop(keys // chunk, project)

    def attend(step):
        h = step // (rows // q_block)
        b = step % (rows // q_block)
        here = pl.ds(pl.multiple_of(b * q_block, q_block), q_block)
        q = q_ref[h, here, :]
        top = jnp.full((q_block, 1), -jnp.inf, F32)
        acc = jnp.zeros((q_block, LANES), F32)
        for j in range(keys // k_block):
            at = slice(j * k_block, (j + 1) * k_block)
            s = lax.dot_general(
                q, k_buf[h, at, :], (((1,), (1,)), ((), ())), preferred_element_type=F32
            )
            new_top = jnp.maximum(top, jnp.max(s, axis=-1, keepdims=True))
            p = jnp.exp2((s - new_top) * scale).astype(BF)
            pv = jnp.dot(p, v_buf[h, at, :], preferred_element_type=F32)
            if j == 0:
                acc = pv
            else:
                acc = acc * jnp.exp2((top - new_top) * scale) + pv
            top = new_top
        out_ref[h, here, :] = (acc[:, :VDIM] / acc[:, VDIM : VDIM + 1]).astype(BF)

    loop(heads * (rows // q_block), attend)
    tokens.to_sibling()
    tokens.finish()


def gather_sems(n_ep, n_tp):
    dma = pltpu.SemaphoreType.DMA
    blocks = n_ep // 2 * n_tp
    return [dma, dma((n_ep * n_tp,)), dma((n_ep // 2,)), dma((blocks,)), dma((blocks,))]


def attention(n_ep, n_tp, sent, tok, q, w):
    heads, rows, _ = q.shape
    part = sent.shape[0]
    n = n_ep * n_tp
    keys = part * n
    flops = 4 * heads * rows * keys * 256
    vmem = pl.BlockSpec(memory_space=pltpu.VMEM)
    return pl.pallas_call(
        functools.partial(attention_kernel, heads, n_ep, n_tp),
        out_shape=(
            jax.ShapeDtypeStruct((heads, rows, VDIM), BF),
            jax.ShapeDtypeStruct((n,) + tok.shape, BF),
        ),
        in_specs=[vmem] * 4,
        out_specs=(vmem, vmem),
        scratch_shapes=[
            pltpu.VMEM((n,) + sent.shape, BF),
            pltpu.VMEM((heads, keys, LANES), BF),
            pltpu.VMEM((heads, keys, LANES), BF),
        ]
        + gather_sems(n_ep, n_tp)
        + gather_sems(n_ep, n_tp),
        compiler_params=pltpu.CompilerParams(
            vmem_limit_bytes=60 * 1024 * 1024, collective_id=0, has_side_effects=True
        ),
        cost_estimate=pl.CostEstimate(
            flops=flops, bytes_accessed=8 * 1024 * 1024, transcendentals=heads * rows * keys
        ),
        name="attention",
    )(sent, tok, q, w)


def experts_kernel(
    n_ep,
    n_tp,
    att_ref,
    wo_ref,
    piece_ref,
    scale_ref,
    own_ref,
    wg_hbm,
    wu_hbm,
    wd_hbm,
    mix_ref,
    exp_ref,
    wg,
    wu,
    wd,
    hid,
    p_send,
    p_recv,
    t_send,
    t_recv,
    e_send,
    e_recv,
    w_sem,
    ps,
    pr,
    ts,
    tr,
    es,
    er,
):
    ep, t = lax.axis_index("ep"), lax.axis_index("tp")
    part = mix_ref.shape[0]
    total, share = t_send.shape[1:]
    room = e_send.shape[1]
    loads = [
        pltpu.make_async_copy(a, b, w_sem.at[i])
        for i, (a, b) in enumerate(((wg_hbm, wg), (wu_hbm, wu), (wd_hbm, wd)))
    ]
    for load in loads:
        load.start()
    greet(n_ep, n_tp, True)

    def to_tp(send, recv, ss, rs, d):
        to = (t + d) % n_tp
        return remote(send.at[to], recv.at[t], ss.at[d], rs.at[t], ep, to)

    def from_tp(send, recv, ss, rs, d):
        frm = (t + n_tp - d) % n_tp
        remote(send.at[frm], recv.at[frm], ss.at[0], rs.at[frm], ep, frm).wait_recv()
        return frm

    mixer = (p_send, p_recv, ps, pr)
    terms = (t_send, t_recv, ts, tr)

    def project(d):
        to = (t + d) % n_tp
        rows = att_ref[pl.ds(pl.multiple_of(to * part, part), part), :]
        p_send[to] = jnp.dot(rows, wo_ref[...], preferred_element_type=F32).astype(BF)

        @pl.when(d < n_tp)
        def _():
            to_tp(*mixer, d).start()

    loop(n_tp + 1, project, 1)

    step = 256
    loads[0].wait()
    loads[1].wait()

    def up(c):
        at = pl.ds(pl.multiple_of(c * step, step), step)
        g = jnp.dot(piece_ref[...], wg[:, at], preferred_element_type=F32)
        u = jnp.dot(piece_ref[...], wu[:, at], preferred_element_type=F32)
        hid[:, at] = (g / (1.0 + jnp.exp(-g)) * u).astype(BF)

    loop(hid.shape[1] // step, up)
    loads[2].wait()

    def down(d):
        to = (t + d) % n_tp
        at = pl.ds(pl.multiple_of(to * share, share), share)
        t_send[to] = jnp.dot(hid[...], wd[:, at], preferred_element_type=F32).astype(BF)

        @pl.when(d < n_tp)
        def _():
            to_tp(*terms, d).start()

    loop(n_tp + 1, down, 1)

    def reduced(send, group):
        acc = send[t].astype(F32)
        for d in range(1, n_tp):
            frm = from_tp(*group, d)
            acc = acc + group[1][frm].astype(F32)
        return acc

    mix_ref[...] = reduced(p_send, mixer).astype(BF)
    out = (reduced(t_send, terms) * scale_ref[:, :1]).astype(BF)
    e_send[...] = out.reshape(n_ep, room, share)
    e_recv[ep] = e_send[ep]

    def to_ep(d):
        to = (ep + d) % n_ep
        return remote(e_send.at[to], e_recv.at[ep], es.at[d], er.at[ep], to, t)

    loop(n_ep, lambda d: to_ep(d).start(), 1)

    def arrived(d):
        frm = (ep + n_ep - d) % n_ep
        remote(e_send.at[frm], e_recv.at[frm], es.at[0], er.at[frm], frm, t).wait_recv()

    loop(n_ep, arrived, 1)
    back = e_recv[...].reshape(n_ep * room, share)
    exp_ref[...] = jnp.dot(own_ref[...], back, preferred_element_type=F32).astype(BF)

    def drain(d):
        to_tp(*mixer, d).wait_send()
        to_tp(*terms, d).wait_send()

    loop(n_tp, drain, 1)
    loop(n_ep, lambda d: to_ep(d).wait_send(), 1)


def experts(n_ep, n_tp, room, att, w_out, piece, scale, own, w_gate, w_up, w_down):
    vmem = pl.BlockSpec(memory_space=pltpu.VMEM)
    hbm = pl.BlockSpec(memory_space=pl.ANY)
    dma = pltpu.SemaphoreType.DMA
    width = w_out.shape[1]
    total = piece.shape[0]
    part, share = att.shape[0] // n_tp, width // n_tp
    flops = 6 * total * width * w_gate.shape[1] + 2 * att.shape[0] * att.shape[1] * width
    return pl.pallas_call(
        functools.partial(experts_kernel, n_ep, n_tp),
        out_shape=(
            jax.ShapeDtypeStruct((part, width), BF),
            jax.ShapeDtypeStruct((own.shape[0], share), BF),
        ),
        in_specs=[vmem] * 5 + [hbm] * 3,
        out_specs=(vmem, vmem),
        scratch_shapes=[
            pltpu.VMEM(w_gate.shape, BF),
            pltpu.VMEM(w_up.shape, BF),
            pltpu.VMEM(w_down.shape, BF),
            pltpu.VMEM((total, w_gate.shape[1]), BF),
            pltpu.VMEM((n_tp, part, width), BF),
            pltpu.VMEM((n_tp, part, width), BF),
            pltpu.VMEM((n_tp, total, share), BF),
            pltpu.VMEM((n_tp, total, share), BF),
            pltpu.VMEM((n_ep, room, share), BF),
            pltpu.VMEM((n_ep, room, share), BF),
            dma((3,)),
            dma((n_tp,)),
            dma((n_tp,)),
            dma((n_tp,)),
            dma((n_tp,)),
            dma((n_ep,)),
            dma((n_ep,)),
        ],
        compiler_params=pltpu.CompilerParams(
            vmem_limit_bytes=60 * 1024 * 1024, collective_id=1, has_side_effects=True
        ),
        cost_estimate=pl.CostEstimate(
            flops=flops, bytes_accessed=20 * 1024 * 1024, transcendentals=0
        ),
        name="experts",
    )(att, w_out, piece, scale, own, w_gate, w_up, w_down)


def lay_heads(weights, heads, width, offset):
    depth = weights.shape[0]
    split = weights.reshape(depth, heads, width)
    return jnp.pad(split, ((0, 0), (0, 0), (offset, LANES - width - offset)))


def shards(
    q_latent,
    kv_latent,
    rope_key,
    q_gain,
    kv_gain,
    w_q_nope,
    w_q_rope,
    w_k_nope,
    w_value,
    w_out,
    tokens_b,
    norm_gain_b,
    routes,
    route_logits,
    w_gate,
    w_up,
    w_down,
):
    n_ep = lax.axis_size("ep")
    n_tp = lax.axis_size("tp")
    e_at = lax.axis_index("ep")
    t_at = lax.axis_index("tp")
    own_rows = q_latent.shape[0]
    heads = w_q_nope.shape[1] // NOPE
    rows_b = tokens_b.shape[0]
    width = tokens_b.shape[1]
    half = ROPE // 2

    part = own_rows // n_tp
    kv_part = lax.dynamic_slice_in_dim(kv_latent, t_at * part, part, 0)
    rope_part = lax.dynamic_slice_in_dim(rope_key, t_at * part, part, 0).astype(F32)
    places = e_at * own_rows + t_at * part + jnp.arange(part, dtype=jnp.int32)
    cosine, sine = angle_tables(places)
    first, second = rope_part[:, :half], rope_part[:, half:]
    sent = jnp.concatenate(
        [
            rms_rows(kv_part, kv_gain),
            jnp.zeros((part, NOPE), BF),
            (first * cosine - second * sine).astype(BF),
            (first * sine + second * cosine).astype(BF),
            jnp.zeros((part, LANES - NOPE - ROPE), BF),
        ],
        axis=1,
    )

    part_b = rows_b // n_tp
    tok_part = lax.dynamic_slice_in_dim(tokens_b, t_at * part_b, part_b, 0)
    route_part = lax.dynamic_slice_in_dim(routes, t_at * part_b, part_b, 0)
    logit_part = lax.dynamic_slice_in_dim(route_logits, t_at * part_b, part_b, 0)
    weights_b = jax.nn.softmax(logit_part, axis=-1)
    high = weights_b.astype(BF)
    low = (weights_b - high.astype(F32)).astype(BF)
    extra = jnp.concatenate(
        [route_part.astype(BF), high, low, jnp.zeros((part_b, LANES - 6), BF)], axis=1
    )
    sent_b = jnp.concatenate([rms_rows(tok_part, norm_gain_b), extra], axis=1)

    q_normed = rms_rows(q_latent, q_gain)
    w_nope = lay_heads(w_q_nope, heads, NOPE, 0)
    w_rope = lay_heads(w_q_rope, heads, ROPE, NOPE)
    turn = w_q_rope.reshape(-1, heads, ROPE)
    turned = jnp.concatenate([-turn[..., half:], turn[..., :half]], axis=-1)
    w_turned = jnp.pad(turned, ((0, 0), (0, 0), (NOPE, LANES - NOPE - ROPE)))
    cos_q, sin_q = angle_tables(e_at * own_rows + jnp.arange(own_rows, dtype=jnp.int32))
    ones = jnp.ones((own_rows, NOPE), F32)
    tail = jnp.zeros((own_rows, LANES - NOPE - ROPE), F32)
    cos_row = jnp.concatenate([ones, cos_q, cos_q, tail], axis=1)
    sin_row = jnp.concatenate([0.0 * ones, sin_q, sin_q, tail], axis=1)
    plain = jnp.einsum("rd,dhl->hrl", q_normed, w_nope + w_rope, preferred_element_type=F32)
    swapped = jnp.einsum("rd,dhl->hrl", q_normed, w_turned, preferred_element_type=F32)
    q = (plain * cos_row + swapped * sin_row).astype(BF)

    w_keys = lay_heads(w_k_nope, heads, NOPE, 0).reshape(-1, heads * LANES)
    w_vals = lay_heads(w_value, heads, VDIM, 0).reshape(-1, heads * LANES)
    w_kv = jnp.concatenate([w_keys, w_vals], axis=1)
    attended, tok_all = attention(n_ep, n_tp, sent, sent_b, q, w_kv)
    attended = attended.transpose(1, 0, 2).reshape(own_rows, heads * VDIM)
    tok_all = tok_all.reshape(n_ep * rows_b, width + LANES)

    room = -(-(3 * rows_b // n_ep) // 16) * 16
    total_b = tok_all.shape[0]
    info = tok_all[:, width : width + LANES].astype(F32)
    me = e_at.astype(F32)
    hit_0 = (info[:, 0] == me).astype(F32)
    hit_1 = (info[:, 1] == me).astype(F32)
    hit = hit_0 + hit_1
    weight = hit_0 * (info[:, 2] + info[:, 4]) + hit_1 * (info[:, 3] + info[:, 5])
    order = jnp.arange(rows_b)
    before = (order[:, None] < order[None, :]).astype(BF)
    slot = jnp.dot(hit.reshape(n_ep, rows_b).astype(BF), before, preferred_element_type=F32)
    row = slot + (jnp.arange(n_ep, dtype=F32) * room)[:, None]
    row = jnp.where(hit > 0, row.reshape(total_b), -1.0)
    index = jnp.arange(n_ep * room, dtype=F32)
    chosen = index[:, None] == row[None, :]
    pick = chosen.astype(BF)
    row_weight = jnp.sum(jnp.where(chosen, weight[None, :], 0.0), axis=1, keepdims=True)
    piece = jnp.dot(pick, tok_all[:, :width], preferred_element_type=F32).astype(BF)
    named = (routes[:, :, None] == jnp.arange(n_ep, dtype=jnp.int32)).astype(F32)
    used = jnp.sum(named, axis=1)
    ahead = jnp.dot(before.T, used.astype(BF), preferred_element_type=F32)
    own = (ahead[:, :, None] == jnp.arange(room, dtype=F32)) & (used[:, :, None] > 0)
    own = own.astype(BF).reshape(rows_b, n_ep * room)
    scale = jnp.broadcast_to(row_weight, (n_ep * room, LANES))
    mixer_out, expert_mix = experts(
        n_ep, n_tp, room, attended, w_out, piece, scale, own, w_gate[0], w_up[0], w_down[0]
    )
    return (mixer_out, expert_mix)


def solution(mesh):
    placed = (
        P("ep", None),
        P("ep", None),
        P("ep", None),
        P(),
        P(),
        P(None, "tp"),
        P(None, "tp"),
        P(None, "tp"),
        P(None, "tp"),
        P("tp", None),
        P("ep", None),
        P(),
        P("ep", None),
        P("ep", None),
        P("ep", None, "tp"),
        P("ep", None, "tp"),
        P("ep", "tp", None),
    )
    return jax.shard_map(
        shards,
        mesh=mesh,
        in_specs=placed,
        out_specs=(P(("ep", "tp"), None), P("ep", "tp")),
        check_vma=False,
    )
```

```python
import functools
import math

import jax
import jax.numpy as jnp
from jax import lax
from jax.experimental import pallas as pl
from jax.experimental.pallas import tpu as pltpu
from jax.sharding import PartitionSpec as P

NOPE = 64
ROPE = 32
VDIM = 64
LANES = 128
EPSILON = 1e-06
BF = jnp.bfloat16
F32 = jnp.float32


def rms_rows(values, gain):
    wide = values.astype(F32)
    scaled = wide * lax.rsqrt(jnp.mean(wide * wide, axis=-1, keepdims=True) + EPSILON)
    return (scaled * gain.astype(F32)).astype(BF)


def angle_tables(places):
    half = ROPE // 2
    freqs = 10000.0 ** (-jnp.arange(half, dtype=F32) / half)
    angles = places.astype(F32)[:, None] * freqs[None, :]
    return jnp.cos(angles), jnp.sin(angles)


MESH = pl.DeviceIdType.MESH


def remote(src, dst, send, recv, ep, tp):
    return pltpu.make_async_remote_copy(
        src_ref=src,
        dst_ref=dst,
        send_sem=send,
        recv_sem=recv,
        device_id={"ep": ep, "tp": tp},
        device_id_type=MESH,
    )


def loop(count, body, start=0):
    def step(i, c):
        body(i)
        return c

    lax.fori_loop(start, count, step, 0)


class Gather:
    def __init__(self, n_ep, n_tp, own, buf, local, recv, send_z, send_t, send_c):
        self.n_tp, self.nz = n_tp, n_ep // 2
        self.own, self.buf, self.local = own, buf, local
        self.recv, self.send_z, self.send_t, self.send_c = recv, send_z, send_t, send_c
        ep = lax.axis_index("ep")
        self.z, self.core, self.t = ep // 2, ep % 2, lax.axis_index("tp")
        self.ep = ep

    def slot(self, z, core, t):
        return (z * 2 + core) * self.n_tp + t

    def at_z(self, d):
        return (self.z + self.nz - d) % self.nz

    def at_t(self, d):
        return (self.t + self.n_tp - d) % self.n_tp

    def copy_z(self, d):
        me = self.slot(self.z, self.core, self.t)
        to = (self.z + d) % self.nz
        return remote(
            self.own, self.buf.at[me], self.send_z.at[d], self.recv.at[me], to * 2 + self.core, self.t
        )

    def copy_t(self, dz, d):
        s = self.slot(self.at_z(dz), self.core, self.t)
        to = (self.t + d) % self.n_tp
        return remote(
            self.buf.at[s], self.buf.at[s], self.send_t.at[dz * self.n_tp + d], self.recv.at[s], self.ep, to
        )

    def copy_c(self, dz, d):
        s = self.slot(self.at_z(dz), self.core, self.at_t(d))
        return remote(
            self.buf.at[s],
            self.buf.at[s],
            self.send_c.at[dz * self.n_tp + d],
            self.recv.at[s],
            self.z * 2 + 1 - self.core,
            self.t,
        )

    def landed(self, s):
        remote(self.own, self.buf.at[s], self.local, self.recv.at[s], self.ep, self.t).wait_recv()

    def start(self):
        loop(self.nz, lambda d: self.copy_z(d).start(), 1)
        me = self.slot(self.z, self.core, self.t)
        mine = pltpu.make_async_copy(self.own, self.buf.at[me], self.local)
        mine.start()
        mine.wait()

    def over_tp(self):
        def one(dz):
            @pl.when(dz > 0)
            def _():
                self.landed(self.slot(self.at_z(dz), self.core, self.t))

            loop(self.n_tp, lambda d: self.copy_t(dz, d).start(), 1)
            self.copy_c(dz, 0).start()

        loop(self.nz, one)

    def to_sibling(self):
        def one(dz):
            def inner(d):
                self.landed(self.slot(self.at_z(dz), self.core, self.at_t(d)))
                self.copy_c(dz, d).start()

            loop(self.n_tp, inner, 1)

        loop(self.nz, one)

    def finish(self):
        def one(dz):
            def inner(d):
                self.landed(self.slot(self.at_z(dz), 1 - self.core, self.at_t(d)))
                self.copy_c(dz, d).wait_send()

            loop(self.n_tp, inner)
            loop(self.n_tp, lambda d: self.copy_t(dz, d).wait_send(), 1)

        loop(self.nz, one)
        loop(self.nz, lambda d: self.copy_z(d).wait_send(), 1)


def greet(n_ep, n_tp, every_ep):
    ep, t = lax.axis_index("ep"), lax.axis_index("tp")
    barrier = pltpu.get_barrier_semaphore()

    def hello(e, tp):
        pl.semaphore_signal(barrier, inc=1, device_id={"ep": e, "tp": tp}, device_id_type=MESH)

    loop(n_tp, lambda d: hello(ep, (t + d) % n_tp), 1)
    if every_ep:
        loop(n_ep, lambda d: hello((ep + d) % n_ep, t), 1)
        pl.semaphore_wait(barrier, n_tp + n_ep - 2)
    else:
        nz = n_ep // 2
        loop(nz, lambda d: hello((ep // 2 + d) % nz * 2 + ep % 2, t), 1)
        hello(ep // 2 * 2 + 1 - ep % 2, t)
        pl.semaphore_wait(barrier, n_tp + nz - 1)


def attention_kernel(
    heads,
    n_ep,
    n_tp,
    sent_ref,
    tok_ref,
    lat_ref,
    gain_ref,
    cos_ref,
    sin_ref,
    qn_ref,
    qr_ref,
    wk_ref,
    wv_ref,
    out_ref,
    tok_out,
    kv_buf,
    k_buf,
    v_buf,
    q_ref,
    w_ref,
    *sems,
):
    part, lat = sent_ref.shape[0], wk_ref.shape[0]
    keys = n_ep * n_tp * part
    rows = lat_ref.shape[0]
    scale = (NOPE + ROPE) ** (-0.5) * math.log2(math.e)
    q_block = min(256, rows)
    k_block = 1024
    wide = heads * LANES
    latents = Gather(n_ep, n_tp, sent_ref, kv_buf, *sems[:5])
    tokens = Gather(n_ep, n_tp, tok_ref, tok_out, *sems[5:])
    greet(n_ep, n_tp, False)
    latents.start()
    latents.over_tp()
    tokens.start()

    def beside(parts, depth, width):
        filler = jnp.zeros((depth, LANES - width), BF)
        return jnp.concatenate(parts + [filler], axis=1)

    for h in range(heads):
        nope, value = slice(h * NOPE, (h + 1) * NOPE), slice(h * VDIM, (h + 1) * VDIM)
        w_ref[:, h * LANES : (h + 1) * LANES] = beside([wk_ref[:, nope]], lat, NOPE)
        w_ref[:, wide + h * LANES : wide + (h + 1) * LANES] = beside([wv_ref[:, value]], lat, VDIM)
    normed = rms_rows(lat_ref[...], gain_ref[...])
    deep, half = lat_ref.shape[1], ROPE // 2
    for h in range(heads):
        turn = qr_ref[:, h * ROPE : (h + 1) * ROPE]
        plain = beside([qn_ref[:, h * NOPE : (h + 1) * NOPE], turn], deep, NOPE + ROPE)
        blank = jnp.zeros((deep, NOPE), BF)
        turned = beside([blank, -turn[:, half:], turn[:, :half]], deep, NOPE + ROPE)
        q = jnp.dot(normed, plain, preferred_element_type=F32) * cos_ref[...]
        q = q + jnp.dot(normed, turned, preferred_element_type=F32) * sin_ref[...]
        q_ref[h] = q.astype(BF)
    latents.to_sibling()
    latents.finish()
    tokens.over_tp()
    group = max(1, 512 // part)
    chunk = group * part

    def project(c):
        here = pl.ds(pl.multiple_of(c * chunk, chunk), chunk)
        block = kv_buf[pl.ds(c * group, group)].reshape(chunk, kv_buf.shape[2])
        up = jnp.dot(block[:, :lat], w_ref[...], preferred_element_type=F32)
        turned = block[:, lat:].astype(F32)
        lane = lax.broadcasted_iota(jnp.int32, (chunk, LANES), 1)
        for h in range(heads):
            k_buf[h, here, :] = (up[:, h * LANES : (h + 1) * LANES] + turned).astype(BF)
            v = up[:, wide + h * LANES : wide + (h + 1) * LANES]
            v_buf[h, here, :] = jnp.where(lane < VDIM, v, 1.0).astype(BF)

    loop(keys // chunk, project)

    def attend_head(h, here):
        q = q_ref[h, here, :]
        top, acc = None, None
        for j in range(keys // k_block):
            at = slice(j * k_block, (j + 1) * k_block)
            s = lax.dot_general(
                q, k_buf[h, at, :], (((1,), (1,)), ((), ())), preferred_element_type=F32
            )
            new_top = jnp.max(s, axis=-1, keepdims=True)
            if j > 0:
                new_top = jnp.maximum(top, new_top)
            p = jnp.exp2((s - new_top) * scale).astype(BF)
            pv = jnp.dot(p, v_buf[h, at, :], preferred_element_type=F32)
            acc = pv if j == 0 else acc * jnp.exp2((top - new_top) * scale) + pv
            top = new_top
        return (acc[:, :VDIM] / acc[:, VDIM : VDIM + 1]).astype(BF)

    def attend(step):
        here = pl.ds(pl.multiple_of(step * q_block, q_block), q_block)
        done = [attend_head(h, here) for h in range(heads)]
        out_ref[here, :] = done[0] if heads == 1 else jnp.concatenate(done, axis=1)

    loop(rows // q_block, attend)
    tokens.to_sibling()
    tokens.finish()


def gather_sems(n_ep, n_tp):
    dma = pltpu.SemaphoreType.DMA
    blocks = n_ep // 2 * n_tp
    return [dma, dma((n_ep * n_tp,)), dma((n_ep // 2,)), dma((blocks,)), dma((blocks,))]


def attention(n_ep, n_tp, heads, *operands):
    sent, tok, latent = operands[:3]
    rows = latent.shape[0]
    part = sent.shape[0]
    n = n_ep * n_tp
    keys = part * n
    flops = 4 * heads * rows * keys * 256
    vmem = pl.BlockSpec(memory_space=pltpu.VMEM)
    return pl.pallas_call(
        functools.partial(attention_kernel, heads, n_ep, n_tp),
        out_shape=(
            jax.ShapeDtypeStruct((rows, heads * VDIM), BF),
            jax.ShapeDtypeStruct((n,) + tok.shape, BF),
        ),
        in_specs=[vmem] * len(operands),
        out_specs=(vmem, vmem),
        scratch_shapes=[
            pltpu.VMEM((n,) + sent.shape, BF),
            pltpu.VMEM((heads, keys, LANES), BF),
            pltpu.VMEM((heads, keys, LANES), BF),
            pltpu.VMEM((heads, rows, LANES), BF),
            pltpu.VMEM((operands[-1].shape[0], 2 * heads * LANES), BF),
        ]
        + gather_sems(n_ep, n_tp)
        + gather_sems(n_ep, n_tp),
        compiler_params=pltpu.CompilerParams(
            vmem_limit_bytes=60 * 1024 * 1024, collective_id=0, has_side_effects=True
        ),
        cost_estimate=pl.CostEstimate(
            flops=flops, bytes_accessed=8 * 1024 * 1024, transcendentals=heads * rows * keys
        ),
        name="attention",
    )(*operands)


def experts_kernel(
    n_ep,
    n_tp,
    att_ref,
    wo_ref,
    pick_ref,
    scale_ref,
    own_ref,
    wg_hbm,
    wu_hbm,
    wd_hbm,
    tok_hbm,
    mix_ref,
    exp_ref,
    wg,
    wu,
    wd,
    tok,
    piece_ref,
    hid,
    p_send,
    p_recv,
    t_send,
    t_recv,
    e_send,
    e_recv,
    w_sem,
    ps,
    pr,
    ts,
    tr,
    es,
    er,
):
    ep, t = lax.axis_index("ep"), lax.axis_index("tp")
    part = mix_ref.shape[0]
    total, share = t_send.shape[1:]
    room = e_send.shape[1]
    loads = [
        pltpu.make_async_copy(a, b, w_sem.at[i])
        for i, (a, b) in enumerate(
            ((tok_hbm, tok), (wg_hbm, wg), (wu_hbm, wu), (wd_hbm, wd))
        )
    ]
    for load in loads:
        load.start()
    greet(n_ep, n_tp, True)

    def to_tp(send, recv, ss, rs, d):
        to = (t + d) % n_tp
        return remote(send.at[to], recv.at[t], ss.at[d], rs.at[t], ep, to)

    def from_tp(send, recv, ss, rs, d):
        frm = (t + n_tp - d) % n_tp
        remote(send.at[frm], recv.at[frm], ss.at[0], rs.at[frm], ep, frm).wait_recv()
        return frm

    mixer = (p_send, p_recv, ps, pr)
    terms = (t_send, t_recv, ts, tr)

    def project(d):
        to = (t + d) % n_tp
        rows = att_ref[pl.ds(pl.multiple_of(to * part, part), part), :]
        p_send[to] = jnp.dot(rows, wo_ref[...], preferred_element_type=F32).astype(BF)

        @pl.when(d < n_tp)
        def _():
            to_tp(*mixer, d).start()

    loop(n_tp + 1, project, 1)

    loads[0].wait()
    span = 512

    def select(c):
        at = pl.ds(pl.multiple_of(c * span, span), span)
        rows = jnp.dot(pick_ref[...], tok[:, at], preferred_element_type=F32)
        piece_ref[:, at] = rows.astype(BF)

    loop(piece_ref.shape[1] // span, select)
    step = 256
    loads[1].wait()
    loads[2].wait()

    def up(c):
        at = pl.ds(pl.multiple_of(c * step, step), step)
        g = jnp.dot(piece_ref[...], wg[:, at], preferred_element_type=F32)
        u = jnp.dot(piece_ref[...], wu[:, at], preferred_element_type=F32)
        hid[:, at] = (g / (1.0 + jnp.exp(-g)) * u).astype(BF)

    loop(hid.shape[1] // step, up)
    loads[3].wait()

    def down(d):
        to = (t + d) % n_tp
        at = pl.ds(pl.multiple_of(to * share, share), share)
        t_send[to] = jnp.dot(hid[...], wd[:, at], preferred_element_type=F32).astype(BF)

        @pl.when(d < n_tp)
        def _():
            to_tp(*terms, d).start()

    loop(n_tp + 1, down, 1)

    def reduced(send, group):
        acc = send[t].astype(F32)
        for d in range(1, n_tp):
            frm = from_tp(*group, d)
            acc = acc + group[1][frm].astype(F32)
        return acc

    mix_ref[...] = reduced(p_send, mixer).astype(BF)
    out = (reduced(t_send, terms) * scale_ref[:, :1]).astype(BF)
    e_send[...] = out.reshape(n_ep, room, share)
    e_recv[ep] = e_send[ep]

    def to_ep(d):
        to = (ep + d) % n_ep
        return remote(e_send.at[to], e_recv.at[ep], es.at[d], er.at[ep], to, t)

    loop(n_ep, lambda d: to_ep(d).start(), 1)

    def arrived(d):
        frm = (ep + n_ep - d) % n_ep
        remote(e_send.at[frm], e_recv.at[frm], es.at[0], er.at[frm], frm, t).wait_recv()

    loop(n_ep, arrived, 1)
    back = e_recv[...].reshape(n_ep * room, share)
    exp_ref[...] = jnp.dot(own_ref[...], back, preferred_element_type=F32).astype(BF)

    def drain(d):
        to_tp(*mixer, d).wait_send()
        to_tp(*terms, d).wait_send()

    loop(n_tp, drain, 1)
    loop(n_ep, lambda d: to_ep(d).wait_send(), 1)


def experts(n_ep, n_tp, room, att, w_out, pick, scale, own, w_gate, w_up, w_down, tok):
    vmem = pl.BlockSpec(memory_space=pltpu.VMEM)
    hbm = pl.BlockSpec(memory_space=pl.ANY)
    dma = pltpu.SemaphoreType.DMA
    width = w_out.shape[1]
    total = pick.shape[0]
    part, share = att.shape[0] // n_tp, width // n_tp
    flops = 6 * total * width * w_gate.shape[1] + 2 * att.shape[0] * att.shape[1] * width
    return pl.pallas_call(
        functools.partial(experts_kernel, n_ep, n_tp),
        out_shape=(
            jax.ShapeDtypeStruct((part, width), BF),
            jax.ShapeDtypeStruct((own.shape[0], share), BF),
        ),
        in_specs=[vmem] * 5 + [hbm] * 4,
        out_specs=(vmem, vmem),
        scratch_shapes=[
            pltpu.VMEM(w_gate.shape, BF),
            pltpu.VMEM(w_up.shape, BF),
            pltpu.VMEM(w_down.shape, BF),
            pltpu.VMEM(tok.shape, BF),
            pltpu.VMEM((total, width), BF),
            pltpu.VMEM((total, w_gate.shape[1]), BF),
            pltpu.VMEM((n_tp, part, width), BF),
            pltpu.VMEM((n_tp, part, width), BF),
            pltpu.VMEM((n_tp, total, share), BF),
            pltpu.VMEM((n_tp, total, share), BF),
            pltpu.VMEM((n_ep, room, share), BF),
            pltpu.VMEM((n_ep, room, share), BF),
            dma((4,)),
            dma((n_tp,)),
            dma((n_tp,)),
            dma((n_tp,)),
            dma((n_tp,)),
            dma((n_ep,)),
            dma((n_ep,)),
        ],
        compiler_params=pltpu.CompilerParams(
            vmem_limit_bytes=60 * 1024 * 1024, collective_id=1, has_side_effects=True
        ),
        cost_estimate=pl.CostEstimate(
            flops=flops, bytes_accessed=20 * 1024 * 1024, transcendentals=0
        ),
        name="experts",
    )(att, w_out, pick, scale, own, w_gate, w_up, w_down, tok)


def shards(
    q_latent,
    kv_latent,
    rope_key,
    q_gain,
    kv_gain,
    w_q_nope,
    w_q_rope,
    w_k_nope,
    w_value,
    w_out,
    tokens_b,
    norm_gain_b,
    routes,
    route_logits,
    w_gate,
    w_up,
    w_down,
):
    n_ep = lax.axis_size("ep")
    n_tp = lax.axis_size("tp")
    e_at = lax.axis_index("ep")
    t_at = lax.axis_index("tp")
    own_rows = q_latent.shape[0]
    heads = w_q_nope.shape[1] // NOPE
    rows_b = tokens_b.shape[0]
    width = tokens_b.shape[1]
    half = ROPE // 2

    part = own_rows // n_tp
    kv_part = lax.dynamic_slice_in_dim(kv_latent, t_at * part, part, 0)
    rope_part = lax.dynamic_slice_in_dim(rope_key, t_at * part, part, 0).astype(F32)
    places = e_at * own_rows + t_at * part + jnp.arange(part, dtype=jnp.int32)
    cosine, sine = angle_tables(places)
    first, second = rope_part[:, :half], rope_part[:, half:]
    sent = jnp.concatenate(
        [
            rms_rows(kv_part, kv_gain),
            jnp.zeros((part, NOPE), BF),
            (first * cosine - second * sine).astype(BF),
            (first * sine + second * cosine).astype(BF),
            jnp.zeros((part, LANES - NOPE - ROPE), BF),
        ],
        axis=1,
    )

    part_b = rows_b // n_tp
    tok_part = lax.dynamic_slice_in_dim(tokens_b, t_at * part_b, part_b, 0)
    route_part = lax.dynamic_slice_in_dim(routes, t_at * part_b, part_b, 0)
    logit_part = lax.dynamic_slice_in_dim(route_logits, t_at * part_b, part_b, 0)
    weights_b = jax.nn.softmax(logit_part, axis=-1)
    high = weights_b.astype(BF)
    low = (weights_b - high.astype(F32)).astype(BF)
    extra = jnp.concatenate(
        [route_part.astype(BF), high, low, jnp.zeros((part_b, LANES - 6), BF)], axis=1
    )
    sent_b = jnp.concatenate([rms_rows(tok_part, norm_gain_b), extra], axis=1)

    cos_q, sin_q = angle_tables(e_at * own_rows + jnp.arange(own_rows, dtype=jnp.int32))
    ones = jnp.ones((own_rows, NOPE), F32)
    tail = jnp.zeros((own_rows, LANES - NOPE - ROPE), F32)
    cos_row = jnp.concatenate([ones, cos_q, cos_q, tail], axis=1)
    sin_row = jnp.concatenate([0.0 * ones, sin_q, sin_q, tail], axis=1)
    attended, tok_all = attention(
        n_ep,
        n_tp,
        heads,
        sent,
        sent_b,
        q_latent,
        q_gain[None, :],
        cos_row,
        sin_row,
        w_q_nope,
        w_q_rope,
        w_k_nope,
        w_value,
    )
    tok_all = tok_all.reshape(n_ep * rows_b, width + LANES)

    room = -(-(3 * rows_b // n_ep) // 16) * 16
    total_b = tok_all.shape[0]
    info = tok_all[:, width : width + LANES].astype(F32)
    me = e_at.astype(F32)
    hit_0 = (info[:, 0] == me).astype(F32)
    hit_1 = (info[:, 1] == me).astype(F32)
    hit = hit_0 + hit_1
    weight = hit_0 * (info[:, 2] + info[:, 4]) + hit_1 * (info[:, 3] + info[:, 5])
    order = jnp.arange(rows_b)
    before = (order[:, None] < order[None, :]).astype(BF)
    slot = jnp.dot(hit.reshape(n_ep, rows_b).astype(BF), before, preferred_element_type=F32)
    row = slot + (jnp.arange(n_ep, dtype=F32) * room)[:, None]
    row = jnp.where(hit > 0, row.reshape(total_b), -1.0)
    index = jnp.arange(n_ep * room, dtype=F32)
    chosen = index[:, None] == row[None, :]
    pick = chosen.astype(BF)
    row_weight = jnp.sum(jnp.where(chosen, weight[None, :], 0.0), axis=1, keepdims=True)
    named = (routes[:, :, None] == jnp.arange(n_ep, dtype=jnp.int32)).astype(F32)
    used = jnp.sum(named, axis=1)
    ahead = jnp.dot(before.T, used.astype(BF), preferred_element_type=F32)
    own = (ahead[:, :, None] == jnp.arange(room, dtype=F32)) & (used[:, :, None] > 0)
    own = own.astype(BF).reshape(rows_b, n_ep * room)
    scale = jnp.broadcast_to(row_weight, (n_ep * room, LANES))
    mixer_out, expert_mix = experts(
        n_ep, n_tp, room, attended, w_out, pick, scale, own, w_gate[0], w_up[0], w_down[0], tok_all
    )
    return (mixer_out, expert_mix)


def solution(mesh):
    placed = (
        P("ep", None),
        P("ep", None),
        P("ep", None),
        P(),
        P(),
        P(None, "tp"),
        P(None, "tp"),
        P(None, "tp"),
        P(None, "tp"),
        P("tp", None),
        P("ep", None),
        P(),
        P("ep", None),
        P("ep", None),
        P("ep", None, "tp"),
        P("ep", None, "tp"),
        P("ep", "tp", None),
    )
    return jax.shard_map(
        shards,
        mesh=mesh,
        in_specs=placed,
        out_specs=(P(("ep", "tp"), None), P("ep", "tp")),
        check_vma=False,
    )
```

```python
import functools
import math

import jax
import jax.numpy as jnp
from jax import lax
from jax.experimental import pallas as pl
from jax.experimental.pallas import tpu as pltpu
from jax.sharding import PartitionSpec as P

NOPE = 64
ROPE = 32
VDIM = 64
LANES = 128
EPSILON = 1e-06
BF = jnp.bfloat16
F32 = jnp.float32


def rms_rows(values, gain):
    wide = values.astype(F32)
    scaled = wide * lax.rsqrt(jnp.mean(wide * wide, axis=-1, keepdims=True) + EPSILON)
    return (scaled * gain.astype(F32)).astype(BF)


def angle_tables(places):
    half = ROPE // 2
    freqs = 10000.0 ** (-jnp.arange(half, dtype=F32) / half)
    angles = places.astype(F32)[:, None] * freqs[None, :]
    return jnp.cos(angles), jnp.sin(angles)


MESH = pl.DeviceIdType.MESH


def remote(src, dst, send, recv, ep, tp):
    return pltpu.make_async_remote_copy(
        src_ref=src,
        dst_ref=dst,
        send_sem=send,
        recv_sem=recv,
        device_id={"ep": ep, "tp": tp},
        device_id_type=MESH,
    )


def loop(count, body, start=0):
    def step(i, c):
        body(i)
        return c

    lax.fori_loop(start, count, step, 0)


class Gather:
    def __init__(self, n_ep, n_tp, own, buf, local, recv, send_z, send_t, send_c):
        self.n_tp, self.nz = n_tp, n_ep // 2
        self.own, self.buf, self.local = own, buf, local
        self.square = n_tp == 4
        self.direct = 3 if self.square else n_tp
        self.recv, self.send_z, self.send_t, self.send_c = recv, send_z, send_t, send_c
        ep = lax.axis_index("ep")
        self.z, self.core, self.t = ep // 2, ep % 2, lax.axis_index("tp")
        self.ep = ep

    def slot(self, z, core, t):
        return (z * 2 + core) * self.n_tp + t

    def at_z(self, d):
        return (self.z + self.nz - d) % self.nz

    def at_t(self, d, back=True):
        if self.square:
            return (self.t // 2 + d // 2) % 2 * 2 + (self.t % 2 + d % 2) % 2
        return (self.t + (self.n_tp - d if back else d)) % self.n_tp

    def copy_z(self, d):
        me = self.slot(self.z, self.core, self.t)
        to = (self.z + d) % self.nz
        return remote(
            self.own, self.buf.at[me], self.send_z.at[d], self.recv.at[me], to * 2 + self.core, self.t
        )

    def copy_t(self, dz, d):
        s = self.slot(self.at_z(dz), self.core, self.t)
        to = self.at_t(d, False)
        return remote(
            self.buf.at[s], self.buf.at[s], self.send_t.at[dz * self.n_tp + d], self.recv.at[s], self.ep, to
        )

    def relay(self, dz):
        s = self.slot(self.at_z(dz), self.core, self.at_t(1 + dz % 2))
        to = self.at_t(2 - dz % 2)
        return remote(
            self.buf.at[s], self.buf.at[s], self.send_t.at[dz * self.n_tp + 3], self.recv.at[s], self.ep, to
        )

    def copy_c(self, dz, d):
        s = self.slot(self.at_z(dz), self.core, self.at_t(d))
        return remote(
            self.buf.at[s],
            self.buf.at[s],
            self.send_c.at[dz * self.n_tp + d],
            self.recv.at[s],
            self.z * 2 + 1 - self.core,
            self.t,
        )

    def landed(self, s):
        remote(self.own, self.buf.at[s], self.local, self.recv.at[s], self.ep, self.t).wait_recv()

    def start(self):
        loop(self.nz, lambda d: self.copy_z(d).start(), 1)
        me = self.slot(self.z, self.core, self.t)
        mine = pltpu.make_async_copy(self.own, self.buf.at[me], self.local)
        mine.start()
        mine.wait()

    def over_tp(self):
        def one(dz):
            @pl.when(dz > 0)
            def _():
                self.landed(self.slot(self.at_z(dz), self.core, self.t))

            loop(self.direct, lambda d: self.copy_t(dz, d).start(), 1)
            self.copy_c(dz, 0).start()

        loop(self.nz, one)

    def to_sibling(self):
        def one(dz):
            def inner(d):
                self.landed(self.slot(self.at_z(dz), self.core, self.at_t(d)))
                self.copy_c(dz, d).start()

            loop(self.direct, inner, 1)
            if self.square:
                self.relay(dz).start()

        loop(self.nz, one)

    def last(self):
        def one(dz):
            self.landed(self.slot(self.at_z(dz), self.core, self.at_t(3)))
            self.copy_c(dz, 3).start()

        if self.square:
            loop(self.nz, one)

    def finish(self):
        def one(dz):
            def inner(d):
                self.landed(self.slot(self.at_z(dz), 1 - self.core, self.at_t(d)))
                self.copy_c(dz, d).wait_send()

            loop(self.n_tp, inner)
            loop(self.direct, lambda d: self.copy_t(dz, d).wait_send(), 1)
            if self.square:
                self.relay(dz).wait_send()

        loop(self.nz, one)
        loop(self.nz, lambda d: self.copy_z(d).wait_send(), 1)


def greet(n_ep, n_tp, every_ep):
    ep, t = lax.axis_index("ep"), lax.axis_index("tp")
    barrier = pltpu.get_barrier_semaphore()

    def hello(e, tp):
        pl.semaphore_signal(barrier, inc=1, device_id={"ep": e, "tp": tp}, device_id_type=MESH)

    loop(n_tp, lambda d: hello(ep, (t + d) % n_tp), 1)
    if every_ep:
        loop(n_ep, lambda d: hello((ep + d) % n_ep, t), 1)
        pl.semaphore_wait(barrier, n_tp + n_ep - 2)
    else:
        nz = n_ep // 2
        loop(nz, lambda d: hello((ep // 2 + d) % nz * 2 + ep % 2, t), 1)
        hello(ep // 2 * 2 + 1 - ep % 2, t)
        pl.semaphore_wait(barrier, n_tp + nz - 1)


def attention_kernel(
    heads,
    n_ep,
    n_tp,
    sent_ref,
    tok_ref,
    lat_ref,
    gain_ref,
    cos_ref,
    sin_ref,
    qn_ref,
    qr_ref,
    wk_ref,
    wv_ref,
    out_ref,
    tok_out,
    kv_buf,
    k_buf,
    v_buf,
    q_ref,
    w_ref,
    *sems,
):
    part, lat = sent_ref.shape[0], wk_ref.shape[0]
    keys = n_ep * n_tp * part
    rows = lat_ref.shape[0]
    scale = (NOPE + ROPE) ** (-0.5) * math.log2(math.e)
    q_block = min(256, rows)
    k_block = 1024
    wide = heads * LANES
    latents = Gather(n_ep, n_tp, sent_ref, kv_buf, *sems[:5])
    tokens = Gather(n_ep, n_tp, tok_ref, tok_out, *sems[5:])
    greet(n_ep, n_tp, False)
    latents.start()
    latents.over_tp()
    tokens.start()

    def beside(parts, depth, width):
        filler = jnp.zeros((depth, LANES - width), BF)
        return jnp.concatenate(parts + [filler], axis=1)

    for h in range(heads):
        nope, value = slice(h * NOPE, (h + 1) * NOPE), slice(h * VDIM, (h + 1) * VDIM)
        w_ref[:, h * LANES : (h + 1) * LANES] = beside([wk_ref[:, nope]], lat, NOPE)
        w_ref[:, wide + h * LANES : wide + (h + 1) * LANES] = beside([wv_ref[:, value]], lat, VDIM)
    normed = rms_rows(lat_ref[...], gain_ref[...])
    deep, half = lat_ref.shape[1], ROPE // 2
    for h in range(heads):
        turn = qr_ref[:, h * ROPE : (h + 1) * ROPE]
        plain = beside([qn_ref[:, h * NOPE : (h + 1) * NOPE], turn], deep, NOPE + ROPE)
        blank = jnp.zeros((deep, NOPE), BF)
        turned = beside([blank, -turn[:, half:], turn[:, :half]], deep, NOPE + ROPE)
        q = jnp.dot(normed, plain, preferred_element_type=F32) * cos_ref[...]
        q = q + jnp.dot(normed, turned, preferred_element_type=F32) * sin_ref[...]
        q_ref[h] = q.astype(BF)
    latents.to_sibling()
    latents.last()
    latents.finish()
    tokens.over_tp()
    group = max(1, 512 // part)
    chunk = group * part

    def project(c):
        here = pl.ds(pl.multiple_of(c * chunk, chunk), chunk)
        block = kv_buf[pl.ds(c * group, group)].reshape(chunk, kv_buf.shape[2])
        up = jnp.dot(block[:, :lat], w_ref[...], preferred_element_type=F32)
        turned = block[:, lat:].astype(F32)
        lane = lax.broadcasted_iota(jnp.int32, (chunk, LANES), 1)
        for h in range(heads):
            k_buf[h, here, :] = (up[:, h * LANES : (h + 1) * LANES] + turned).astype(BF)
            v = up[:, wide + h * LANES : wide + (h + 1) * LANES]
            v_buf[h, here, :] = jnp.where(lane < VDIM, v, 1.0).astype(BF)

    loop(keys // chunk, project)

    def attend_head(h, here):
        q = q_ref[h, here, :]
        top, acc = None, None
        for j in range(keys // k_block):
            at = slice(j * k_block, (j + 1) * k_block)
            s = lax.dot_general(
                q, k_buf[h, at, :], (((1,), (1,)), ((), ())), preferred_element_type=F32
            )
            new_top = jnp.max(s, axis=-1, keepdims=True)
            if j > 0:
                new_top = jnp.maximum(top, new_top)
            p = jnp.exp2((s - new_top) * scale).astype(BF)
            pv = jnp.dot(p, v_buf[h, at, :], preferred_element_type=F32)
            acc = pv if j == 0 else acc * jnp.exp2((top - new_top) * scale) + pv
            top = new_top
        return (acc[:, :VDIM] / acc[:, VDIM : VDIM + 1]).astype(BF)

    def attend(step):
        here = pl.ds(pl.multiple_of(step * q_block, q_block), q_block)
        done = [attend_head(h, here) for h in range(heads)]
        out_ref[here, :] = done[0] if heads == 1 else jnp.concatenate(done, axis=1)

        @pl.when(step == max(rows // q_block // 2 - 1, 0))
        def _():
            tokens.to_sibling()

    loop(rows // q_block, attend)
    tokens.last()
    tokens.finish()


def gather_sems(n_ep, n_tp):
    dma = pltpu.SemaphoreType.DMA
    blocks = n_ep // 2 * n_tp
    return [dma, dma((n_ep * n_tp,)), dma((n_ep // 2,)), dma((blocks,)), dma((blocks,))]


def attention(n_ep, n_tp, heads, *operands):
    sent, tok, latent = operands[:3]
    rows = latent.shape[0]
    part = sent.shape[0]
    n = n_ep * n_tp
    keys = part * n
    flops = 4 * heads * rows * keys * 256
    vmem = pl.BlockSpec(memory_space=pltpu.VMEM)
    return pl.pallas_call(
        functools.partial(attention_kernel, heads, n_ep, n_tp),
        out_shape=(
            jax.ShapeDtypeStruct((rows, heads * VDIM), BF),
            jax.ShapeDtypeStruct((n,) + tok.shape, BF),
        ),
        in_specs=[vmem] * len(operands),
        out_specs=(vmem, vmem),
        scratch_shapes=[
            pltpu.VMEM((n,) + sent.shape, BF),
            pltpu.VMEM((heads, keys, LANES), BF),
            pltpu.VMEM((heads, keys, LANES), BF),
            pltpu.VMEM((heads, rows, LANES), BF),
            pltpu.VMEM((operands[-1].shape[0], 2 * heads * LANES), BF),
        ]
        + gather_sems(n_ep, n_tp)
        + gather_sems(n_ep, n_tp),
        compiler_params=pltpu.CompilerParams(
            vmem_limit_bytes=60 * 1024 * 1024, collective_id=0, has_side_effects=True
        ),
        cost_estimate=pl.CostEstimate(
            flops=flops, bytes_accessed=8 * 1024 * 1024, transcendentals=heads * rows * keys
        ),
        name="attention",
    )(*operands)


def experts_kernel(
    n_ep,
    n_tp,
    att_ref,
    wo_ref,
    pick_ref,
    scale_ref,
    own_ref,
    wg_hbm,
    wu_hbm,
    wd_hbm,
    tok_hbm,
    mix_ref,
    exp_ref,
    wg,
    wu,
    wd,
    tok,
    piece_ref,
    hid,
    p_send,
    p_recv,
    t_send,
    t_recv,
    e_send,
    e_recv,
    w_sem,
    ps,
    pr,
    ts,
    tr,
    es,
    er,
):
    ep, t = lax.axis_index("ep"), lax.axis_index("tp")
    part = mix_ref.shape[0]
    total, share = t_send.shape[1:]
    room = e_send.shape[1]
    loads = [
        pltpu.make_async_copy(a, b, w_sem.at[i])
        for i, (a, b) in enumerate(
            ((tok_hbm, tok), (wg_hbm, wg), (wu_hbm, wu), (wd_hbm, wd))
        )
    ]
    for load in loads:
        load.start()
    greet(n_ep, n_tp, True)

    def to_tp(send, recv, ss, rs, d):
        to = (t + d) % n_tp
        return remote(send.at[to], recv.at[t], ss.at[d], rs.at[t], ep, to)

    def from_tp(send, recv, ss, rs, d):
        frm = (t + n_tp - d) % n_tp
        remote(send.at[frm], recv.at[frm], ss.at[0], rs.at[frm], ep, frm).wait_recv()
        return frm

    mixer = (p_send, p_recv, ps, pr)
    terms = (t_send, t_recv, ts, tr)

    def project(d):
        to = (t + d) % n_tp
        rows = att_ref[pl.ds(pl.multiple_of(to * part, part), part), :]
        p_send[to] = jnp.dot(rows, wo_ref[...], preferred_element_type=F32).astype(BF)

        @pl.when(d < n_tp)
        def _():
            to_tp(*mixer, d).start()

    loop(n_tp + 1, project, 1)

    loads[0].wait()
    span = 512

    def select(c):
        at = pl.ds(pl.multiple_of(c * span, span), span)
        rows = jnp.dot(pick_ref[...], tok[:, at], preferred_element_type=F32)
        piece_ref[:, at] = rows.astype(BF)

    loop(piece_ref.shape[1] // span, select)
    step = 256
    loads[1].wait()
    loads[2].wait()

    def up(c):
        at = pl.ds(pl.multiple_of(c * step, step), step)
        g = jnp.dot(piece_ref[...], wg[:, at], preferred_element_type=F32)
        u = jnp.dot(piece_ref[...], wu[:, at], preferred_element_type=F32)
        hid[:, at] = (g / (1.0 + jnp.exp(-g)) * u).astype(BF)

    loop(hid.shape[1] // step, up)
    loads[3].wait()

    def down(d):
        to = (t + d) % n_tp
        at = pl.ds(pl.multiple_of(to * share, share), share)
        t_send[to] = jnp.dot(hid[...], wd[:, at], preferred_element_type=F32).astype(BF)

        @pl.when(d < n_tp)
        def _():
            to_tp(*terms, d).start()

    loop(n_tp + 1, down, 1)

    def reduced(send, group):
        acc = send[t].astype(F32)
        for d in range(1, n_tp):
            frm = from_tp(*group, d)
            acc = acc + group[1][frm].astype(F32)
        return acc

    mix_ref[...] = reduced(p_send, mixer).astype(BF)
    out = (reduced(t_send, terms) * scale_ref[:, :1]).astype(BF)
    e_send[...] = out.reshape(n_ep, room, share)
    e_recv[ep] = e_send[ep]

    def to_ep(d):
        to = (ep + d) % n_ep
        return remote(e_send.at[to], e_recv.at[ep], es.at[d], er.at[ep], to, t)

    loop(n_ep, lambda d: to_ep(d).start(), 1)

    def arrived(d):
        frm = (ep + n_ep - d) % n_ep
        remote(e_send.at[frm], e_recv.at[frm], es.at[0], er.at[frm], frm, t).wait_recv()

    loop(n_ep, arrived, 1)
    back = e_recv[...].reshape(n_ep * room, share)
    exp_ref[...] = jnp.dot(own_ref[...], back, preferred_element_type=F32).astype(BF)

    def drain(d):
        to_tp(*mixer, d).wait_send()
        to_tp(*terms, d).wait_send()

    loop(n_tp, drain, 1)
    loop(n_ep, lambda d: to_ep(d).wait_send(), 1)


def experts(n_ep, n_tp, room, att, w_out, pick, scale, own, w_gate, w_up, w_down, tok):
    vmem = pl.BlockSpec(memory_space=pltpu.VMEM)
    hbm = pl.BlockSpec(memory_space=pl.ANY)
    dma = pltpu.SemaphoreType.DMA
    width = w_out.shape[1]
    total = pick.shape[0]
    part, share = att.shape[0] // n_tp, width // n_tp
    flops = 6 * total * width * w_gate.shape[1] + 2 * att.shape[0] * att.shape[1] * width
    return pl.pallas_call(
        functools.partial(experts_kernel, n_ep, n_tp),
        out_shape=(
            jax.ShapeDtypeStruct((part, width), BF),
            jax.ShapeDtypeStruct((own.shape[0], share), BF),
        ),
        in_specs=[vmem] * 5 + [hbm] * 4,
        out_specs=(vmem, vmem),
        scratch_shapes=[
            pltpu.VMEM(w_gate.shape, BF),
            pltpu.VMEM(w_up.shape, BF),
            pltpu.VMEM(w_down.shape, BF),
            pltpu.VMEM(tok.shape, BF),
            pltpu.VMEM((total, width), BF),
            pltpu.VMEM((total, w_gate.shape[1]), BF),
            pltpu.VMEM((n_tp, part, width), BF),
            pltpu.VMEM((n_tp, part, width), BF),
            pltpu.VMEM((n_tp, total, share), BF),
            pltpu.VMEM((n_tp, total, share), BF),
            pltpu.VMEM((n_ep, room, share), BF),
            pltpu.VMEM((n_ep, room, share), BF),
            dma((4,)),
            dma((n_tp,)),
            dma((n_tp,)),
            dma((n_tp,)),
            dma((n_tp,)),
            dma((n_ep,)),
            dma((n_ep,)),
        ],
        compiler_params=pltpu.CompilerParams(
            vmem_limit_bytes=60 * 1024 * 1024, collective_id=1, has_side_effects=True
        ),
        cost_estimate=pl.CostEstimate(
            flops=flops, bytes_accessed=20 * 1024 * 1024, transcendentals=0
        ),
        name="experts",
    )(att, w_out, pick, scale, own, w_gate, w_up, w_down, tok)


def shards(
    q_latent,
    kv_latent,
    rope_key,
    q_gain,
    kv_gain,
    w_q_nope,
    w_q_rope,
    w_k_nope,
    w_value,
    w_out,
    tokens_b,
    norm_gain_b,
    routes,
    route_logits,
    w_gate,
    w_up,
    w_down,
):
    n_ep = lax.axis_size("ep")
    n_tp = lax.axis_size("tp")
    e_at = lax.axis_index("ep")
    t_at = lax.axis_index("tp")
    own_rows = q_latent.shape[0]
    heads = w_q_nope.shape[1] // NOPE
    rows_b = tokens_b.shape[0]
    width = tokens_b.shape[1]
    half = ROPE // 2

    part = own_rows // n_tp
    kv_part = lax.dynamic_slice_in_dim(kv_latent, t_at * part, part, 0)
    rope_part = lax.dynamic_slice_in_dim(rope_key, t_at * part, part, 0).astype(F32)
    places = e_at * own_rows + t_at * part + jnp.arange(part, dtype=jnp.int32)
    cosine, sine = angle_tables(places)
    first, second = rope_part[:, :half], rope_part[:, half:]
    sent = jnp.concatenate(
        [
            rms_rows(kv_part, kv_gain),
            jnp.zeros((part, NOPE), BF),
            (first * cosine - second * sine).astype(BF),
            (first * sine + second * cosine).astype(BF),
            jnp.zeros((part, LANES - NOPE - ROPE), BF),
        ],
        axis=1,
    )

    part_b = rows_b // n_tp
    tok_part = lax.dynamic_slice_in_dim(tokens_b, t_at * part_b, part_b, 0)
    route_part = lax.dynamic_slice_in_dim(routes, t_at * part_b, part_b, 0)
    logit_part = lax.dynamic_slice_in_dim(route_logits, t_at * part_b, part_b, 0)
    weights_b = jax.nn.softmax(logit_part, axis=-1)
    high = weights_b.astype(BF)
    low = (weights_b - high.astype(F32)).astype(BF)
    extra = jnp.concatenate(
        [route_part.astype(BF), high, low, jnp.zeros((part_b, LANES - 6), BF)], axis=1
    )
    sent_b = jnp.concatenate([rms_rows(tok_part, norm_gain_b), extra], axis=1)

    cos_q, sin_q = angle_tables(e_at * own_rows + jnp.arange(own_rows, dtype=jnp.int32))
    ones = jnp.ones((own_rows, NOPE), F32)
    tail = jnp.zeros((own_rows, LANES - NOPE - ROPE), F32)
    cos_row = jnp.concatenate([ones, cos_q, cos_q, tail], axis=1)
    sin_row = jnp.concatenate([0.0 * ones, sin_q, sin_q, tail], axis=1)
    attended, tok_all = attention(
        n_ep,
        n_tp,
        heads,
        sent,
        sent_b,
        q_latent,
        q_gain[None, :],
        cos_row,
        sin_row,
        w_q_nope,
        w_q_rope,
        w_k_nope,
        w_value,
    )
    tok_all = tok_all.reshape(n_ep * rows_b, width + LANES)

    room = -(-(3 * rows_b // n_ep) // 16) * 16
    total_b = tok_all.shape[0]
    info = tok_all[:, width : width + LANES].astype(F32)
    me = e_at.astype(F32)
    hit_0 = (info[:, 0] == me).astype(F32)
    hit_1 = (info[:, 1] == me).astype(F32)
    hit = hit_0 + hit_1
    weight = hit_0 * (info[:, 2] + info[:, 4]) + hit_1 * (info[:, 3] + info[:, 5])
    order = jnp.arange(rows_b)
    before = (order[:, None] < order[None, :]).astype(BF)
    slot = jnp.dot(hit.reshape(n_ep, rows_b).astype(BF), before, preferred_element_type=F32)
    row = slot + (jnp.arange(n_ep, dtype=F32) * room)[:, None]
    row = jnp.where(hit > 0, row.reshape(total_b), -1.0)
    index = jnp.arange(n_ep * room, dtype=F32)
    chosen = index[:, None] == row[None, :]
    pick = chosen.astype(BF)
    row_weight = jnp.sum(jnp.where(chosen, weight[None, :], 0.0), axis=1, keepdims=True)
    named = (routes[:, :, None] == jnp.arange(n_ep, dtype=jnp.int32)).astype(F32)
    used = jnp.sum(named, axis=1)
    ahead = jnp.dot(before.T, used.astype(BF), preferred_element_type=F32)
    own = (ahead[:, :, None] == jnp.arange(room, dtype=F32)) & (used[:, :, None] > 0)
    own = own.astype(BF).reshape(rows_b, n_ep * room)
    scale = jnp.broadcast_to(row_weight, (n_ep * room, LANES))
    mixer_out, expert_mix = experts(
        n_ep, n_tp, room, attended, w_out, pick, scale, own, w_gate[0], w_up[0], w_down[0], tok_all
    )
    return (mixer_out, expert_mix)


def solution(mesh):
    placed = (
        P("ep", None),
        P("ep", None),
        P("ep", None),
        P(),
        P(),
        P(None, "tp"),
        P(None, "tp"),
        P(None, "tp"),
        P(None, "tp"),
        P("tp", None),
        P("ep", None),
        P(),
        P("ep", None),
        P("ep", None),
        P("ep", None, "tp"),
        P("ep", None, "tp"),
        P("ep", "tp", None),
    )
    return jax.shard_map(
        shards,
        mesh=mesh,
        in_specs=placed,
        out_specs=(P(("ep", "tp"), None), P("ep", "tp")),
        check_vma=False,
    )
```
